32 devices in a mesh: ep: 32 (over z, y, x, core).
Axes of the slice: x: 2, y: 2, z: 4, core: 2. Of those that a mesh axis runs over, the one named last changes fastest.
Arguments:
- tokens: bfloat16 [128, 2048], P('ep'), may hold values from -6 to 6
- norm_gain: float32 [2048], replicated, may hold values from 0.1 to 1.9
- routes: int32 [128, 2], P('ep'), may hold values from 0 to 1, all different within a row; in each aligned block of 4 rows (0 to 3, 4 to 7, ...) at most 4 rows name the same one
- route_weight: float32 [128, 2], P('ep'), may hold values from 0.1 to 1
- gate_weight: bfloat16 [2048, 14336], P(None, 'ep'), may hold values from -0.125 to 0.125
- up_weight: bfloat16 [2048, 14336], P(None, 'ep'), may hold values from -0.125 to 0.125
- down_weight: bfloat16 [14336, 2048], P('ep'), may hold values from -0.0625 to 0.0625
Outputs:
- mixed: bfloat16 [128, 2048], P('ep')
The draws below stay inside these ranges and needn't reach their ends.
Inputs may be any that keep to these rules, and one draw needn't show every extreme that they name: `routes`: each row names two different experts of 0 to 1; among the rows of one device no expert is named by more than 4 rows, and in some device one expert is named by exactly 4.
All inputs are finite; a program needn't handle non-finite values.
Results may differ from the reference program's by a relative error of at most 0.0095.
Values may be sent and summed in bfloat16 or wider, within the bound.
A program may use at most 64 MiB of HBM per device.

```python
import math
import jax
import jax.numpy as jnp
import numpy as np
from jax import lax

D = 2048
FF = 7168
TOK_DEV = 4
EXPERTS = 2
TOKENS = 128
MOST = 4
N_EP = 32


def steps_of(stream_key, extent, shards, smallest, top_value):
    def one(position, blocks):
        steps = jax.random.uniform(jax.random.fold_in(jax.random.fold_in(stream_key, 6), position), (blocks,), jnp.float32, smallest / len(shards), top_value / len(shards))
        return jnp.repeat(jnp.exp(steps), extent[position] // blocks).reshape((-1,) + (1,) * (len(extent) - position - 1))

    gain = one(*shards[0])
    for cut in shards[1:]:
        gain = gain * one(*cut)
    return gain


def assign_block(key, own, number, rows, number_of, top, reach, lean):
    sequence = jax.random.permutation(key, number_of)
    packed, ordinary = shares(number_of, rows * top, reach, lean, True), shares(number_of, rows * top, reach, lean, False)
    places = jnp.arange(number_of)

    def named(tallies, turn):
        used = int((tallies > 0).sum())
        fixed = max(1, used // 4)
        shifted = fixed + (places - fixed + turn * (used - fixed)) % max(1, number_of - fixed)
        return jnp.zeros((number_of,), jnp.int32).at[sequence[jnp.where(places < fixed, places, shifted)]].set(jnp.asarray(tallies, jnp.int32))

    tallies = jnp.where(number % 4 == 0, named(packed, number // 4), named(ordinary, number - number // 4 - 1))
    mixed = jax.random.permutation(jax.random.fold_in(own, 3), number_of)
    giver, sink = mixed[0:number_of // 2 * 2:2], mixed[1:number_of // 2 * 2:2]
    margin = jnp.minimum(tallies[giver] - 1, reach - tallies[sink]) // 2
    margin = jnp.where((giver == sequence[0]) | (sink == sequence[0]) | (tallies[sink] == 0), 0, jnp.maximum(margin, 0))
    shifted = jax.random.randint(jax.random.fold_in(own, 4), (number_of // 2,), 0, 1 << 20) % (margin + 1)
    tallies = tallies.at[giver].add(-shifted).at[sink].add(shifted)
    members = jnp.searchsorted(jnp.cumsum(tallies), jnp.arange(rows * top), side="right").astype(jnp.int32)
    grid = members.reshape(top, rows).T
    grid = grid[jax.random.permutation(jax.random.fold_in(own, 1), rows)]
    turn = jax.random.randint(jax.random.fold_in(own, 2), (rows, 1), 0, top)
    return jnp.take_along_axis(grid, (jnp.arange(top)[None, :] + turn) % top, axis=1)


def shares(number_of, total, most, lean, full):
    portions = [(1 << 20) // math.isqrt(standing ** lean) + 1 for standing in range(1, number_of + 1)]
    largest = most if full else min(most, max(-(-total // number_of), total * portions[0] // sum(portions)))
    least = 1 if total - largest >= number_of - 1 else 0
    given, surplus = [largest] + [least] * (number_of - 1), total - largest - least * (number_of - 1)
    while surplus > 0:
        candidates = [i for i in range(1, number_of) if given[i] < largest] or [i for i in range(1, number_of) if given[i] < most]
        mass, left = sum([portions[i] for i in candidates]), surplus
        for i in candidates:
            extra = min(most - given[i], max(1, left * portions[i] // mass), surplus)
            given[i] = given[i] + extra
            surplus = surplus - extra
    return np.array(given)


def gaussian(stream_key, dims, scale, bound, pieces=(), kind=jnp.bfloat16):
    entries = jax.random.normal(stream_key, dims, jnp.float32) * scale
    if len(pieces) > 0:
        entries = steps_of(stream_key, dims, pieces, -0.22, 0.18) * entries
    return jnp.clip(entries, min=-bound, max=bound).astype(kind)


def setup_inputs(seed: int = 0) -> dict:
    key_list = jax.random.split(jax.random.key(seed), 8)
    tokens = gaussian(key_list[0], (TOKENS, D), 1.0, 6.0, ((0, 32),))
    norm_gain = jnp.clip(1.0 + 0.18 * jax.random.normal(key_list[1], (D,), jnp.float32), 0.1, 1.9)
    routes_keys = jax.random.split(jax.random.fold_in(key_list[2], 1), TOKENS // TOK_DEV)
    routes_turns = jax.random.permutation(jax.random.fold_in(key_list[2], 3), TOKENS // TOK_DEV)
    routes = jax.vmap(lambda own, number: assign_block(jax.random.fold_in(key_list[2], 2), own, number, TOK_DEV, EXPERTS, 2, MOST, 2))(routes_keys, routes_turns).reshape((TOKENS, 2))
    route_weight = jnp.clip(0.1 + 0.9 * jax.random.uniform(key_list[3], (TOKENS, 2), jnp.float32) ** steps_of(key_list[3], (TOKENS, 2), ((0, 32),), -0.2, 0.2), 0.1, 1.0)
    gate_weight = gaussian(key_list[4], (D, EXPERTS * FF), D ** -0.5, 0.125, ((1, 32),))
    up_weight = gaussian(key_list[5], (D, EXPERTS * FF), D ** -0.5, 0.125, ((1, 32),))
    down_weight = gaussian(key_list[6], (EXPERTS * FF, D), FF ** -0.5, 0.0625, ((0, 32),))
    return {"tokens": tokens, "norm_gain": norm_gain, "routes": routes, "route_weight": route_weight, "gate_weight": gate_weight, "up_weight": up_weight, "down_weight": down_weight}


epsilon = 1e-06

def expert_rows(rows, gate_part, up_part, down_part):
    gate = jnp.dot(rows, gate_part, preferred_element_type=jnp.float32)
    upper = jnp.dot(rows, up_part, preferred_element_type=jnp.float32)
    hidden = (jax.nn.silu(gate) * upper).astype(jnp.bfloat16)
    return jnp.dot(hidden, down_part, preferred_element_type=jnp.float32)

def reference(tokens, norm_gain, routes, route_weight, gate_weight, up_weight, down_weight):
    values = tokens.astype(jnp.float32)
    scale = lax.rsqrt(lax.optimization_barrier(jnp.mean(values * values, axis=-1, keepdims=True)) + epsilon)
    normed = (values * scale * norm_gain.astype(jnp.float32)).astype(jnp.bfloat16)
    total = tokens.shape[0]
    width = tokens.shape[1]
    flat_experts = routes.reshape(-1).astype(jnp.int32)
    flat_weights = route_weight.reshape(-1).astype(jnp.float32)
    token_of = (jnp.arange(2 * total, dtype=jnp.int32) // 2).astype(jnp.int32)
    expert_ids = jnp.arange(EXPERTS, dtype=jnp.int32)
    onehot = (flat_experts[:, None] == expert_ids[None, :]).astype(jnp.int32)
    ranks = lax.optimization_barrier(jnp.sum((jnp.cumsum(onehot, axis=0) - onehot) * onehot, axis=1)).astype(jnp.int32)
    capacity = N_EP * MOST
    mixed = jnp.zeros((total, width), jnp.float32)
    for expert in range(EXPERTS):
        target = jnp.where(flat_experts == expert, ranks, capacity).astype(jnp.int32)
        rows = jnp.zeros((capacity + 1,), jnp.int32).at[target].set(token_of)[:capacity]
        weights = jnp.zeros((capacity + 1,), jnp.float32).at[target].set(flat_weights)[:capacity]
        gate_part = gate_weight[:, expert * FF:(expert + 1) * FF]
        up_part = up_weight[:, expert * FF:(expert + 1) * FF]
        down_part = down_weight[expert * FF:(expert + 1) * FF, :]
        result = expert_rows(normed[rows], gate_part, up_part, down_part)
        mixed = mixed.at[rows].add(result * weights[:, None])
    return mixed.astype(jnp.bfloat16)
```

```python
import functools

import jax
import jax.numpy as jnp
from jax import lax
from jax.experimental import pallas as pl
from jax.experimental.pallas import tpu as pltpu
from jax.sharding import PartitionSpec as P

GROUP = 16
CORES = 2
PIECES = 2


epsilon = 1e-06
MESH = pl.DeviceIdType.MESH


def mixture_kernel(
    chips, tok_ref, gain_ref, routes_ref, weight_ref, gate_hbm, up_hbm, down_hbm, out_ref,
    gathered, gate_v, up_v, down_v, rows_v, mine_v, pair_out, pair_in, sums_out, sums_in,
    load_sem, tok_send, tok_recv, fwd_send, fwd_recv, pair_send, pair_recv, sum_send, sum_recv,
):
    tok_count, width = tok_ref.shape
    me = lax.axis_index("ep")
    chip = me // CORES
    core = me % CORES
    partner = chip * CORES + (1 - core)
    piece = width // PIECES
    half = chips * tok_count

    loads = [
        pltpu.make_async_copy(src, dst, load_sem.at[i])
        for i, (src, dst) in enumerate(((gate_hbm, gate_v), (up_hbm, up_v), (down_hbm, down_v)))
    ]
    for load in loads:
        load.start()

    barrier = pltpu.get_barrier_semaphore()
    for k in range(1, chips):
        pl.semaphore_signal(
            barrier, inc=1, device_id=(((chip + k) % chips) * CORES + core,), device_id_type=MESH
        )
    pl.semaphore_signal(barrier, inc=1, device_id=(partner,), device_id_type=MESH)

    values = tok_ref[...].astype(jnp.float32)
    scale = lax.rsqrt(jnp.mean(values * values, axis=-1, keepdims=True) + epsilon)
    gathered[0, chip] = (values * scale * gain_ref[...]).astype(jnp.bfloat16)
    pl.semaphore_wait(barrier, chips)

    def to_partner(src, dst, send, recv):
        return pltpu.make_async_remote_copy(
            src_ref=src, dst_ref=dst, send_sem=send, recv_sem=recv,
            device_id=(partner,), device_id_type=MESH,
        )

    spread = []
    for k in range(1, chips):
        copy = pltpu.make_async_remote_copy(
            src_ref=gathered.at[0, chip], dst_ref=gathered.at[0, chip],
            send_sem=tok_send.at[k], recv_sem=tok_recv.at[k],
            device_id=(((chip + k) % chips) * CORES + core,), device_id_type=MESH,
        )
        copy.start()
        spread.append(copy)
    forward = []
    copy = to_partner(gathered.at[0, chip], gathered.at[1, chip], fwd_send.at[0], fwd_recv.at[0])
    copy.start()
    forward.append(copy)
    for k in range(1, chips):
        spread[k - 1].wait_recv()
        origin = (chip + chips - k) % chips
        copy = to_partner(
            gathered.at[0, origin], gathered.at[1, origin], fwd_send.at[k], fwd_recv.at[k]
        )
        copy.start()
        forward.append(copy)

    def lay_out(color):
        block = gathered[color].astype(jnp.float32).reshape(half, width)
        rows_v[color * half:(color + 1) * half, :] = block.astype(jnp.bfloat16)

    lay_out(0)
    for copy in forward:
        copy.wait_recv()
    lay_out(1)

    rows = rows_v[...]
    loads[0].wait()
    gate = jnp.dot(rows, gate_v[...], preferred_element_type=jnp.float32)
    loads[1].wait()
    upper = jnp.dot(rows, up_v[...], preferred_element_type=jnp.float32)
    hidden = (jax.nn.silu(gate) * upper).astype(jnp.bfloat16)
    loads[2].wait()

    pairs = []
    for c in range(PIECES):
        part = jnp.dot(
            hidden, down_v[:, c * piece:(c + 1) * piece], preferred_element_type=jnp.float32
        )
        mine_v[c] = part[:half]
        pair_out[c] = part[half:].astype(jnp.bfloat16)
        copy = to_partner(pair_out.at[c], pair_in.at[c], pair_send.at[c], pair_recv.at[c])
        copy.start()
        pairs.append(copy)

    results = []
    for c in range(PIECES):
        pairs[c].wait_recv()
        total = mine_v[c] + pair_in[c].astype(jnp.float32)
        sums_out[c] = total.reshape(chips, tok_count, piece).astype(jnp.bfloat16)
        for k in range(1, chips):
            target = (chip + k) % chips
            copy = pltpu.make_async_remote_copy(
                src_ref=sums_out.at[c, target], dst_ref=sums_in.at[c, chip],
                send_sem=sum_send.at[c, k], recv_sem=sum_recv.at[c, k],
                device_id=(target * CORES + core,), device_id_type=MESH,
            )
            copy.start()
            results.append(copy)
        sums_in[c, chip] = sums_out[c, chip]

    experts = chips * CORES // GROUP
    per_expert = chips // experts
    routes = routes_ref[...]
    weights = weight_ref[...]
    shares = [
        jnp.sum(jnp.where(routes == e, weights, 0.0), axis=1, keepdims=True)
        for e in range(experts)
    ]
    for c in range(PIECES):
        for copy in results[c * (chips - 1):(c + 1) * (chips - 1)]:
            copy.wait_recv()
        mixed = jnp.zeros((tok_count, piece), jnp.float32)
        for e in range(experts):
            block = sums_in[c, e * per_expert:(e + 1) * per_expert].astype(jnp.float32)
            mixed = mixed + shares[e] * jnp.sum(block, axis=0)
        out_ref[:, c * piece:(c + 1) * piece] = mixed.astype(jnp.bfloat16)

    for copy in spread + forward + pairs + results:
        copy.wait_send()


def dense_on_device(tokens, norm_gain, routes, route_weight, gate_weight, up_weight, down_weight):
    tok_count, width = tokens.shape
    chips = lax.axis_size("ep") // CORES
    hidden = gate_weight.shape[1]
    vmem = pl.BlockSpec(memory_space=pltpu.VMEM)
    anywhere = pl.BlockSpec(memory_space=pl.ANY)
    half = chips * tok_count
    piece = width // PIECES
    dma = pltpu.SemaphoreType.DMA
    return pl.pallas_call(
        functools.partial(mixture_kernel, chips),
        out_shape=jax.ShapeDtypeStruct((tok_count, width), jnp.bfloat16),
        in_specs=[vmem] * 4 + [anywhere] * 3,
        out_specs=vmem,
        scratch_shapes=[
            pltpu.VMEM((CORES, chips, tok_count, width), jnp.bfloat16),
            pltpu.VMEM((width, hidden), jnp.bfloat16),
            pltpu.VMEM((width, hidden), jnp.bfloat16),
            pltpu.VMEM((hidden, width), jnp.bfloat16),
            pltpu.VMEM((CORES * half, width), jnp.bfloat16),
            pltpu.VMEM((PIECES, half, piece), jnp.float32),
            pltpu.VMEM((PIECES, half, piece), jnp.bfloat16),
            pltpu.VMEM((PIECES, half, piece), jnp.bfloat16),
            pltpu.VMEM((PIECES, chips, tok_count, piece), jnp.bfloat16),
            pltpu.VMEM((PIECES, chips, tok_count, piece), jnp.bfloat16),
            dma((3,)),
            dma((chips,)),
            dma((chips,)),
            dma((chips,)),
            dma((chips,)),
            dma((PIECES,)),
            dma((PIECES,)),
            dma((PIECES, chips)),
            dma((PIECES, chips)),
        ],
        compiler_params=pltpu.CompilerParams(collective_id=0, has_side_effects=True),
    )(
        tokens, norm_gain.reshape(1, width), routes, route_weight,
        gate_weight, up_weight, down_weight,
    )


def expert_rows(rows, gate_part, up_part, down_part):
    gate = jnp.dot(rows, gate_part, preferred_element_type=jnp.float32)
    upper = jnp.dot(rows, up_part, preferred_element_type=jnp.float32)
    hidden = (jax.nn.silu(gate) * upper).astype(jnp.bfloat16)
    return jnp.dot(hidden, down_part, preferred_element_type=jnp.float32)


def normalize(tokens, norm_gain):
    values = tokens.astype(jnp.float32)
    scale = lax.rsqrt(jnp.mean(values * values, axis=-1, keepdims=True) + epsilon)
    return (values * scale * norm_gain).astype(jnp.bfloat16)


def on_device(tokens, norm_gain, routes, route_weight, gate_weight, up_weight, down_weight):
    normed = normalize(tokens, norm_gain)
    tok_count = tokens.shape[0]
    width = tokens.shape[1]
    devices = lax.axis_size("ep")
    experts = devices // GROUP
    most = min(tok_count, max(tok_count // 2, (2 * tok_count + experts - 1) // experts))
    expert_ids = lax.broadcasted_iota(jnp.int32, (1, experts), 1)
    pairs = 2 * tok_count
    flat_experts = routes.reshape(pairs)
    flat_weights = route_weight.reshape(pairs)
    onehot = (flat_experts[:, None] == expert_ids).astype(jnp.int32)
    earlier = jnp.cumsum(onehot, axis=0) - onehot
    slot = jnp.sum(earlier * onehot, axis=1)
    target = flat_experts * most + slot
    slot_ids = lax.broadcasted_iota(jnp.int32, (experts * most, pairs), 0)
    placed = (slot_ids == target[None, :]).astype(jnp.float32)
    pair_rows = lax.broadcasted_iota(jnp.int32, (pairs, tok_count), 0) // 2
    pair_cols = lax.broadcasted_iota(jnp.int32, (pairs, tok_count), 1)
    pair_token = (pair_rows == pair_cols).astype(jnp.float32)
    picker = jnp.dot(placed, pair_token, precision=lax.Precision.HIGHEST)
    outgoing = jnp.dot(
        picker.astype(jnp.bfloat16), normed, preferred_element_type=jnp.float32
    ).astype(jnp.bfloat16)
    outgoing = jnp.broadcast_to(
        outgoing.reshape(experts, 1, most, width), (experts, GROUP, most, width)
    )
    outgoing = outgoing.reshape(devices, most, width)
    received = lax.all_to_all(outgoing, "ep", split_axis=0, concat_axis=0, tiled=True)
    count = received.shape[1]
    flat = received.reshape(devices * count, width)
    result = expert_rows(flat, gate_weight, up_weight, down_weight).reshape(devices, count, width)
    back = lax.all_to_all(result, "ep", split_axis=0, concat_axis=0, tiled=True)
    summed = jnp.sum(back.reshape(experts, GROUP, most, width), axis=1).reshape(
        experts * most, width
    )
    weighted_pairs = pair_token.T * flat_weights[None, :]
    selector = jnp.dot(weighted_pairs, placed.T, precision=lax.Precision.HIGHEST)
    mixed = jnp.dot(selector, summed, precision=lax.Precision.HIGHEST)
    return mixed.astype(jnp.bfloat16)


def solution(mesh):
    every_expert = mesh.shape["ep"] == 2 * GROUP
    return jax.shard_map(
        dense_on_device if every_expert else on_device,
        mesh=mesh,
        in_specs=(
            P("ep", None),
            P(),
            P("ep", None),
            P("ep", None),
            P(None, "ep"),
            P(None, "ep"),
            P("ep", None),
        ),
        out_specs=P("ep", None),
        check_vma=False,
    )
```

```python
import functools

import jax
import jax.numpy as jnp
from jax import lax
from jax.experimental import pallas as pl
from jax.experimental.pallas import tpu as pltpu
from jax.sharding import PartitionSpec as P

GROUP = 16
CORES = 2
PIECES = 1


epsilon = 1e-06
MESH = pl.DeviceIdType.MESH


def times_transposed(rows, part):
    return lax.dot_general(
        rows, part, (((1,), (1,)), ((), ())), preferred_element_type=jnp.float32
    )


def mixture_kernel(
    chips, tok_hbm, gain_hbm, routes_hbm, weight_hbm, gate_hbm, up_hbm, down_hbm, out_ref,
    tok_ref, gain_ref, routes_ref, weight_ref, gathered, gate_v, up_v, down_v, rows_v, mine_v, pair_out, pair_in, sums_out, sums_in,
    load_sem, small_sem, tok_send, tok_recv, fwd_send, fwd_recv, pair_send, pair_recv, sum_send, sum_recv,
):
    tok_count, width = tok_hbm.shape
    me = lax.axis_index("ep")
    chip = me // CORES
    core = me % CORES
    partner = chip * CORES + (1 - core)
    piece = width // PIECES
    half = chips * tok_count

    others = [(chip + k) % chips for k in range(1, chips)]

    def twin(other):
        return (other * CORES + core,)

    small = [
        pltpu.make_async_copy(src, dst, small_sem.at[i])
        for i, (src, dst) in enumerate((
            (tok_hbm, tok_ref), (gain_hbm, gain_ref),
            (routes_hbm, routes_ref), (weight_hbm, weight_ref),
        ))
    ]
    for load in small:
        load.start()
    loads = [
        pltpu.make_async_copy(src, dst, load_sem.at[i])
        for i, (src, dst) in enumerate(((gate_hbm, gate_v), (up_hbm, up_v), (down_hbm, down_v)))
    ]
    barrier = pltpu.get_barrier_semaphore()
    for other in others:
        pl.semaphore_signal(barrier, inc=1, device_id=twin(other), device_id_type=MESH)
    pl.semaphore_signal(barrier, inc=1, device_id=(partner,), device_id_type=MESH)

    for load in loads:
        load.start()
    for load in small:
        load.wait()

    values = tok_ref[...].astype(jnp.float32)
    scale = lax.rsqrt(jnp.mean(values * values, axis=-1, keepdims=True) + epsilon)
    gathered[0, chip] = (values * scale * gain_ref[...]).astype(jnp.bfloat16)
    pl.semaphore_wait(barrier, chips)

    def to_partner(src, dst, send, recv):
        return pltpu.make_async_remote_copy(
            src_ref=src, dst_ref=dst, send_sem=send, recv_sem=recv,
            device_id=(partner,), device_id_type=MESH,
        )

    spread = []
    for other in others:
        copy = pltpu.make_async_remote_copy(
            src_ref=gathered.at[0, chip], dst_ref=gathered.at[0, chip],
            send_sem=tok_send.at[other], recv_sem=tok_recv.at[chip],
            device_id=twin(other), device_id_type=MESH,
        )
        copy.start()
        spread.append(copy)
    forward = []
    copy = to_partner(
        gathered.at[0, chip], gathered.at[1, chip], fwd_send.at[chip], fwd_recv.at[chip]
    )
    copy.start()
    forward.append(copy)
    for other in others[::-1]:
        pltpu.make_async_remote_copy(
            src_ref=gathered.at[0, other], dst_ref=gathered.at[0, other],
            send_sem=tok_send.at[other], recv_sem=tok_recv.at[other],
            device_id=twin(other), device_id_type=MESH,
        ).wait_recv()
        copy = to_partner(
            gathered.at[0, other], gathered.at[1, other], fwd_send.at[other], fwd_recv.at[other]
        )
        copy.start()
        forward.append(copy)

    def lay_out(color):
        block = gathered[color].astype(jnp.float32).reshape(half, width)
        rows_v[color * half:(color + 1) * half, :] = block.astype(jnp.bfloat16)

    lay_out(0)
    for copy in forward:
        copy.wait_recv()
    lay_out(1)

    rows = rows_v[...]
    loads[0].wait()
    gate = times_transposed(rows, gate_v[...])
    loads[1].wait()
    upper = times_transposed(rows, up_v[...])
    hidden = (jax.nn.silu(gate) * upper).astype(jnp.bfloat16)
    loads[2].wait()

    pairs = []
    for c in range(PIECES):
        part = jnp.dot(
            hidden, down_v[:, c * piece:(c + 1) * piece], preferred_element_type=jnp.float32
        )
        mine_v[c] = part[:half]
        pair_out[c] = part[half:].astype(jnp.bfloat16)
        copy = to_partner(pair_out.at[c], pair_in.at[c], pair_send.at[c], pair_recv.at[c])
        copy.start()
        pairs.append(copy)

    results = []
    for c in range(PIECES):
        pairs[c].wait_recv()
        total = mine_v[c] + pair_in[c].astype(jnp.float32)
        sums_out[c] = total.reshape(chips, tok_count, piece).astype(jnp.bfloat16)
        for other in others:
            copy = pltpu.make_async_remote_copy(
                src_ref=sums_out.at[c, other], dst_ref=sums_in.at[c, chip],
                send_sem=sum_send.at[c, other], recv_sem=sum_recv.at[c, chip],
                device_id=twin(other), device_id_type=MESH,
            )
            copy.start()
            results.append(copy)
        sums_in[c, chip] = sums_out[c, chip]

    experts = chips * CORES // GROUP
    per_expert = chips // experts
    routes = routes_ref[...]
    weights = weight_ref[...]
    shares = [
        jnp.sum(jnp.where(routes == e, weights, 0.0), axis=0, keepdims=True).T
        for e in range(experts)
    ]
    for c in range(PIECES):
        for other in others[::-1]:
            pltpu.make_async_remote_copy(
                src_ref=sums_out.at[c, other], dst_ref=sums_in.at[c, other],
                send_sem=sum_send.at[c, other], recv_sem=sum_recv.at[c, other],
                device_id=twin(other), device_id_type=MESH,
            ).wait_recv()
        mixed = jnp.zeros((tok_count, piece), jnp.float32)
        for e in range(experts):
            block = sums_in[c, e * per_expert:(e + 1) * per_expert].astype(jnp.float32)
            mixed = mixed + shares[e] * jnp.sum(block, axis=0)
        out_ref[:, c * piece:(c + 1) * piece] = mixed.astype(jnp.bfloat16)

    for copy in spread + forward + pairs + results:
        copy.wait_send()


def dense_on_device(tokens, norm_gain, routes, route_weight, gate_weight, up_weight, down_weight):
    tok_count, width = tokens.shape
    chips = lax.axis_size("ep") // CORES
    hidden = gate_weight.shape[1]
    vmem = pl.BlockSpec(memory_space=pltpu.VMEM)
    anywhere = pl.BlockSpec(memory_space=pl.ANY)
    half = chips * tok_count
    piece = width // PIECES
    dma = pltpu.SemaphoreType.DMA
    return pl.pallas_call(
        functools.partial(mixture_kernel, chips),
        out_shape=pltpu.VMEM((tok_count, width), jnp.bfloat16),
        in_specs=[anywhere] * 7,
        out_specs=vmem,
        scratch_shapes=[
            pltpu.VMEM((tok_count, width), jnp.bfloat16),
            pltpu.VMEM((1, width), jnp.float32),
            pltpu.VMEM((2, tok_count), jnp.int32),
            pltpu.VMEM((2, tok_count), jnp.float32),
            pltpu.VMEM((CORES, chips, tok_count, width), jnp.bfloat16),
            pltpu.VMEM((hidden, width), jnp.bfloat16),
            pltpu.VMEM((hidden, width), jnp.bfloat16),
            pltpu.VMEM((hidden, width), jnp.bfloat16),
            pltpu.VMEM((CORES * half, width), jnp.bfloat16),
            pltpu.VMEM((PIECES, half, piece), jnp.float32),
            pltpu.VMEM((PIECES, half, piece), jnp.bfloat16),
            pltpu.VMEM((PIECES, half, piece), jnp.bfloat16),
            pltpu.VMEM((PIECES, chips, tok_count, piece), jnp.bfloat16),
            pltpu.VMEM((PIECES, chips, tok_count, piece), jnp.bfloat16),
            dma((3,)),
            dma((4,)),
            dma((chips,)),
            dma((chips,)),
            dma((chips,)),
            dma((chips,)),
            dma((PIECES,)),
            dma((PIECES,)),
            dma((PIECES, chips)),
            dma((PIECES, chips)),
        ],
        compiler_params=pltpu.CompilerParams(collective_id=0, has_side_effects=True),
    )(
        tokens, norm_gain.reshape(1, width), routes.T, route_weight.T,
        gate_weight.T, up_weight.T, down_weight,
    )


def expert_rows(rows, gate_part, up_part, down_part):
    gate = jnp.dot(rows, gate_part, preferred_element_type=jnp.float32)
    upper = jnp.dot(rows, up_part, preferred_element_type=jnp.float32)
    hidden = (jax.nn.silu(gate) * upper).astype(jnp.bfloat16)
    return jnp.dot(hidden, down_part, preferred_element_type=jnp.float32)


def normalize(tokens, norm_gain):
    values = tokens.astype(jnp.float32)
    scale = lax.rsqrt(jnp.mean(values * values, axis=-1, keepdims=True) + epsilon)
    return (values * scale * norm_gain).astype(jnp.bfloat16)


def on_device(tokens, norm_gain, routes, route_weight, gate_weight, up_weight, down_weight):
    normed = normalize(tokens, norm_gain)
    tok_count = tokens.shape[0]
    width = tokens.shape[1]
    devices = lax.axis_size("ep")
    experts = devices // GROUP
    most = min(tok_count, max(tok_count // 2, (2 * tok_count + experts - 1) // experts))
    expert_ids = lax.broadcasted_iota(jnp.int32, (1, experts), 1)
    pairs = 2 * tok_count
    flat_experts = routes.reshape(pairs)
    flat_weights = route_weight.reshape(pairs)
    onehot = (flat_experts[:, None] == expert_ids).astype(jnp.int32)
    earlier = jnp.cumsum(onehot, axis=0) - onehot
    slot = jnp.sum(earlier * onehot, axis=1)
    target = flat_experts * most + slot
    slot_ids = lax.broadcasted_iota(jnp.int32, (experts * most, pairs), 0)
    placed = (slot_ids == target[None, :]).astype(jnp.float32)
    pair_rows = lax.broadcasted_iota(jnp.int32, (pairs, tok_count), 0) // 2
    pair_cols = lax.broadcasted_iota(jnp.int32, (pairs, tok_count), 1)
    pair_token = (pair_rows == pair_cols).astype(jnp.float32)
    picker = jnp.dot(placed, pair_token, precision=lax.Precision.HIGHEST)
    outgoing = jnp.dot(
        picker.astype(jnp.bfloat16), normed, preferred_element_type=jnp.float32
    ).astype(jnp.bfloat16)
    outgoing = jnp.broadcast_to(
        outgoing.reshape(experts, 1, most, width), (experts, GROUP, most, width)
    )
    outgoing = outgoing.reshape(devices, most, width)
    received = lax.all_to_all(outgoing, "ep", split_axis=0, concat_axis=0, tiled=True)
    count = received.shape[1]
    flat = received.reshape(devices * count, width)
    result = expert_rows(flat, gate_weight, up_weight, down_weight).reshape(devices, count, width)
    back = lax.all_to_all(result, "ep", split_axis=0, concat_axis=0, tiled=True)
    summed = jnp.sum(back.reshape(experts, GROUP, most, width), axis=1).reshape(
        experts * most, width
    )
    weighted_pairs = pair_token.T * flat_weights[None, :]
    selector = jnp.dot(weighted_pairs, placed.T, precision=lax.Precision.HIGHEST)
    mixed = jnp.dot(selector, summed, precision=lax.Precision.HIGHEST)
    return mixed.astype(jnp.bfloat16)


def solution(mesh):
    every_expert = mesh.shape["ep"] == 2 * GROUP
    return jax.shard_map(
        dense_on_device if every_expert else on_device,
        mesh=mesh,
        in_specs=(
            P("ep", None),
            P(),
            P("ep", None),
            P("ep", None),
            P(None, "ep"),
            P(None, "ep"),
            P("ep", None),
        ),
        out_specs=P("ep", None),
        check_vma=False,
    )
```
